32 devices in a mesh: ep: 4 (over y, x), tp: 8 (over z, core).
Axes of the slice: x: 2, y: 2, z: 4, core: 2. Of those that a mesh axis runs over, the one named last changes fastest.
Arguments:
- queries: bfloat16 [3072, 2048], P('ep', 'tp'), may hold values from -6 to 6
- values: bfloat16 [3072, 2048], P('ep', 'tp'), may hold values from -6 to 6
- forget_gate_logits: bfloat16 [2, 3072, 2048], P(None, 'ep', 'tp'), may hold values from -5 to 5
- output_gate_logits: bfloat16 [3072, 2048], P('ep', 'tp'), may hold values from -6 to 6
- forget_gate_headroom: float32 [2, 2048], P(None, 'tp'), may hold values from 0 to 0.1, as said below
- spike_log_decay: float32 [3072], P('ep'), may hold values from -1.6 to 0
- head_norm_gain: float32 [2048], P('tp'), may hold values from 0.1 to 1.9
- output_projection: bfloat16 [2048, 2048], P(None, 'tp'), may hold values from -0.125 to 0.125
- second_micro_input: bfloat16 [3072, 2048], P('ep'), may hold values from -170 to 170
- expert_norm_gain: float32 [2048], replicated, may hold values from 0.1 to 1.9
- token_group_index: int32 [3072], P('ep'), may hold values from 0 to 1, as said below
- token_expert_pair: int32 [3072, 2], P('ep'), may hold values from 0 to 3, as said below
- group_router_scores: float32 [3072, 2], P('ep'), may hold values from -6 to 320
- expert_router_scores: float32 [3072, 2], P('ep'), may hold values from -6 to 6
- expert_gate_weight: bfloat16 [8, 2048, 4096], P('ep', None, 'tp'), may hold values from -0.125 to 0.125
- expert_up_weight: bfloat16 [8, 2048, 4096], P('ep', None, 'tp'), may hold values from -0.125 to 0.125
- expert_down_weight: bfloat16 [8, 4096, 2048], P('ep', 'tp'), may hold values from -1.25 to 1.25
Outputs:
- recurrence_output: bfloat16 [3072, 2048], P('ep', 'tp')
- expert_tokens: bfloat16 [3072, 2048], P('ep', 'tp')
The draws below stay inside these ranges and needn't reach their ends.
Inputs may be any that keep to these rules, and one draw needn't show every extreme that they name: `token_group_index`: within the rows of one device each of the 2 groups is named by the same number of rows. The two entries of a row differ. Within the rows of one device every expert token_group_index * 4 + token_expert_pair is named exactly 192 times. `forget_gate_headroom`: Positive.
All inputs are finite; a program needn't handle non-finite values.
Results may differ from the reference program's by a relative error of at most 0.018.
Values may be sent and summed in bfloat16 or wider, within the bound.
A program may use at most 128 MiB of HBM per device.

```python
import math
import jax
import jax.numpy as jnp
from jax import lax

D = 2048
HEADS = 16
HEAD_DIM = 128
HG = 2048
FF = 4096
GROUP_EXP = 4
EXPERTS = 8
GROUPS = 2
BLOCK = 64
TOK_EP = 768
MICRO_TOKENS = 3072
N_TP = 8


def draw_forget_gate_logits(key, part):
    base_key, shift_key = jax.random.split(jax.random.fold_in(key, 3))
    block_count = MICRO_TOKENS // TOK_EP
    shifts = jax.random.uniform(shift_key, (2, block_count, 1, 1), jnp.float32, -1.5, 1.5)
    noise_part = jax.random.normal(base_key, (2, block_count, TOK_EP, HG), jnp.float32)
    return jnp.clip(noise_part + shifts, -5.0, 5.0).reshape(2, MICRO_TOKENS, HG).astype(jnp.bfloat16)


def draw_forget_gate_headroom(key, part):
    head_key, slow_key, fast_key, chan_key = jax.random.split(jax.random.fold_in(key, 5), 4)
    fast_head = jax.random.randint(head_key, (2, HEADS, 1), 0, 2) == 1
    slow_gap = jax.random.uniform(slow_key, (2, HEADS, 1), jnp.float32, 0.2, 1.0) / MICRO_TOKENS
    fast_gap = jax.random.uniform(fast_key, (2, HEADS, 1), jnp.float32, 0.04, 0.1)
    spread = jax.random.uniform(chan_key, (2, HEADS, HEAD_DIM), jnp.float32, 0.7, 1.0)
    return (jnp.where(fast_head, fast_gap, slow_gap) * spread).reshape(2, HG).astype(jnp.float32)


def draw_spike_log_decay(key, part):
    position_random_key, strength_random_key = jax.random.split(jax.random.fold_in(key, 9))
    spike_positions = jax.random.randint(position_random_key, (3,), 0, MICRO_TOKENS)
    spike_strength = jax.random.uniform(strength_random_key, (3,), jnp.float32, math.log(0.6), math.log(0.8))
    spike_position_mask = jnp.arange(MICRO_TOKENS)[:, None] == spike_positions[None, :]
    return jnp.sum(jnp.where(spike_position_mask, spike_strength[None, :], 0.0), axis=1).astype(jnp.float32)


def draw_second_micro_input(key, part):
    noise_key, row_key, col_key = jax.random.split(jax.random.fold_in(key, 13), 3)
    row_scale = jnp.exp(jax.random.uniform(row_key, (MICRO_TOKENS, 1), jnp.float32, 0.0, math.log(10.0)))
    col_scale = jnp.exp(jax.random.uniform(col_key, (1, D), jnp.float32, 0.0, math.log(10.0)))
    noise_part = jax.random.normal(noise_key, (MICRO_TOKENS, D), jnp.float32)
    return (jnp.clip(noise_part, -5.0, 5.0) * row_scale * col_scale / 3.0).astype(jnp.bfloat16)


def draw_group_router_scores(key, part):
    base_key = jax.random.fold_in(jax.random.fold_in(key, 17), 0)
    return jnp.clip(1.5 * jax.random.normal(base_key, (MICRO_TOKENS, GROUPS), jnp.float32), -6.0, 6.0)


def block_perm(block_key):
    return jax.random.permutation(block_key, TOK_EP)


def route_table(key):
    perm_key, shift_key = jax.random.split(jax.random.fold_in(key, 23))
    block_count = MICRO_TOKENS // TOK_EP
    places = jax.vmap(block_perm)(jax.random.split(perm_key, block_count)).astype(jnp.int32)
    group_ids = places % GROUPS
    within = places // GROUPS
    shifts = jax.random.randint(shift_key, (block_count, GROUPS), 1, GROUP_EXP)
    step_size = jnp.take_along_axis(shifts, group_ids, axis=1)
    first_inner = within % GROUP_EXP
    second_inner = (within + step_size) % GROUP_EXP
    inner_ids = jnp.stack([first_inner, second_inner], -1).reshape(MICRO_TOKENS, 2)
    return (group_ids.reshape(MICRO_TOKENS).astype(jnp.int32), inner_ids.astype(jnp.int32))


def draw_token_group_index(key, part):
    return route_table(key)[0]


def draw_token_expert_pair(key, part):
    return route_table(key)[1]


def with_spikes(array, rng, source, target, blocks, factor):
    owner, partner = [(jnp.arange(array.shape[axis_at]) // (array.shape[axis_at] // blocks)).reshape([-1 if axis == axis_at else 1 for axis in range(array.ndim)]) for axis_at in (source, target)]
    chosen = jax.random.permutation(rng, blocks)[partner]
    strong = (owner == chosen) | (owner == (partner + blocks // 2) % blocks)
    return jnp.where(strong, factor * array, array)


def shard_levels(stream_key, extent, shards, smallest, high):
    gain, own = 1.0, jax.random.fold_in(stream_key, 6)
    for dim, parts in shards:
        steps = jnp.exp(jax.random.uniform(jax.random.fold_in(own, dim), (parts,), jnp.float32, smallest / len(shards), high / len(shards)))
        gain = gain * jnp.repeat(steps, extent[dim] // parts).reshape([-1 if axis == dim else 1 for axis in range(len(extent))])
    return gain


def scatter_about(rng, dims, deviation, most, shards=(), kind=jnp.bfloat16):
    array = jax.random.normal(rng, dims, jnp.float32) * deviation
    if len(shards) > 0:
        array = shard_levels(rng, dims, shards, -0.22, 0.18) * array
    return jnp.clip(array, min=-most, max=most).astype(kind)


def noise_with(key, extent, scale, most, shards, heavy, held_as=jnp.bfloat16):
    drawn = scale * jax.random.normal(key, extent, jnp.float32)
    if shards:
        drawn = drawn * shard_levels(key, extent, shards, -0.22, 0.18)
    return jnp.clip(with_spikes(drawn, jax.random.fold_in(key, 3), *heavy), -most, most).astype(held_as)


def setup_inputs(seed: int = 0) -> dict:
    arg_keys = jax.random.split(jax.random.key(seed), 18)
    queries = scatter_about(arg_keys[0], (MICRO_TOKENS, HG), 1.0, 6.0, ((0, 4), (1, 8)))
    values = scatter_about(arg_keys[1], (MICRO_TOKENS, HG), 1.0, 6.0, ((0, 4), (1, 8)))
    forget_gate_logits = draw_forget_gate_logits(jax.random.fold_in(arg_keys[17], 71), 0)
    output_gate_logits = scatter_about(arg_keys[3], (MICRO_TOKENS, HG), 1.0, 6.0, ((0, 4), (1, 8)))
    forget_gate_headroom = draw_forget_gate_headroom(jax.random.fold_in(arg_keys[17], 71), 0)
    spike_log_decay = draw_spike_log_decay(jax.random.fold_in(arg_keys[17], 71), 0)
    head_norm_gain = jnp.clip(1.0 + 0.18 * jax.random.normal(arg_keys[6], (HG,), jnp.float32), 0.1, 1.9)
    output_projection = scatter_about(arg_keys[7], (HG, D), HG ** -0.5, 0.125, ((1, 8),))
    second_micro_input = draw_second_micro_input(jax.random.fold_in(arg_keys[17], 71), 0)
    expert_norm_gain = jnp.clip(1.0 + 0.18 * jax.random.normal(arg_keys[9], (D,), jnp.float32), 0.1, 1.9)
    token_group_index = draw_token_group_index(jax.random.fold_in(arg_keys[17], 71), 0)
    token_expert_pair = draw_token_expert_pair(jax.random.fold_in(arg_keys[17], 71), 0)
    group_router_scores = draw_group_router_scores(jax.random.fold_in(arg_keys[17], 71), 0)
    expert_router_scores = scatter_about(arg_keys[13], (MICRO_TOKENS, 2), 1.5, 6.0, ((0, 4),), jnp.float32)
    expert_gate_weight = scatter_about(arg_keys[14], (EXPERTS, D, FF), D ** -0.5, 0.125, ((0, 4), (2, 8)))
    expert_up_weight = scatter_about(arg_keys[15], (EXPERTS, D, FF), D ** -0.5, 0.125, ((0, 4), (2, 8)))
    expert_down_weight = noise_with(arg_keys[16], (EXPERTS, FF, D), (4.0 * FF ** -0.5), 1.25, ((0, 4), (1, 8)), (1, 2, 8, 2.0))
    return dict(queries=queries, values=values, forget_gate_logits=forget_gate_logits, output_gate_logits=output_gate_logits, forget_gate_headroom=forget_gate_headroom, spike_log_decay=spike_log_decay, head_norm_gain=head_norm_gain, output_projection=output_projection, second_micro_input=second_micro_input, expert_norm_gain=expert_norm_gain, token_group_index=token_group_index, token_expert_pair=token_expert_pair, group_router_scores=group_router_scores, expert_router_scores=expert_router_scores, expert_gate_weight=expert_gate_weight, expert_up_weight=expert_up_weight, expert_down_weight=expert_down_weight)


HEAD_EPS = 1e-06
NORM_EPS = 1e-05
FULL_PRECISION = lax.Precision.HIGHEST

def decay_pieces(forget_gate_logits, forget_gate_headroom, spike_log_decay):
    logits = forget_gate_logits.astype(jnp.float32)
    gap_span = forget_gate_headroom[:, None, :]
    logarithm_decay = jnp.logaddexp(jnp.log1p(-gap_span), jnp.log(gap_span) + jax.nn.log_sigmoid(logits))
    logarithm_decay = logarithm_decay + spike_log_decay[None, :, None]
    key_contributions = gap_span * jax.nn.sigmoid(-logits)
    return (logarithm_decay, key_contributions)

def recurrence(lifted, key_contributions, logarithm_decay, inputs_f):
    length = lifted.shape[0]

    def blocked(tensor):
        return tensor.reshape(length // BLOCK, BLOCK, HEADS, HEAD_DIM)
    causal = jnp.tril(jnp.ones((BLOCK, BLOCK), bool))[:, :, None, None]

    def block_step(carried_state, packed):
        block_of_queries, block_of_keys, decay_block, block_of_values = packed
        running_state = jnp.cumsum(decay_block, axis=0)
        spread = running_state[:, None] - running_state[None, :]
        weight = jnp.where(causal, jnp.exp(jnp.where(causal, spread, 0.0)), 0.0)
        scores = lax.optimization_barrier(jnp.sum(block_of_queries[:, None] * block_of_keys[None, :] * weight, axis=-1))
        inner_out = jnp.einsum('tsh,shv->thv', scores, block_of_values, precision=FULL_PRECISION)
        across_block_output = jnp.einsum('gwm,wma->gwa', block_of_queries * jnp.exp(running_state), carried_state, precision=FULL_PRECISION)
        final_block_row = running_state[-1]
        written_output = jnp.einsum('qnx,qnb->nxb', block_of_keys * jnp.exp(final_block_row[None] - running_state), block_of_values, precision=FULL_PRECISION)
        return (jnp.exp(final_block_row)[:, :, None] * carried_state + written_output, inner_out + across_block_output)
    zero_state = jnp.zeros((HEADS, HEAD_DIM, HEAD_DIM), jnp.float32)
    scanned = lax.scan(block_step, zero_state, (blocked(lifted), blocked(key_contributions), blocked(logarithm_decay), blocked(inputs_f)))
    return scanned[1].reshape(length, HEADS, HEAD_DIM)

def recurrence_portion(queries, values, forget_gate_logits, output_gate_logits, forget_gate_headroom, spike_log_decay, head_norm_gain, output_projection):
    length = queries.shape[0]
    logarithm_decay, key_contributions = decay_pieces(forget_gate_logits, forget_gate_headroom, spike_log_decay)

    def heads_of(tensor):
        return tensor.reshape(length, HEADS, HEAD_DIM)
    lifted = heads_of(jax.nn.silu(queries.astype(jnp.float32)))
    inputs_f = heads_of(values.astype(jnp.float32))
    forward_out = recurrence(lifted, heads_of(key_contributions[0]), heads_of(logarithm_decay[0]), inputs_f)
    backward_out = jnp.flip(recurrence(jnp.flip(lifted, 0), jnp.flip(heads_of(key_contributions[1]), 0), jnp.flip(heads_of(logarithm_decay[1]), 0), jnp.flip(inputs_f, 0)), 0)
    joined = forward_out + backward_out
    normed = joined * lax.rsqrt(lax.optimization_barrier(jnp.mean(joined * joined, -1, keepdims=True)) + HEAD_EPS)
    readout = (normed.reshape(length, HG) * head_norm_gain * jax.nn.silu(output_gate_logits.astype(jnp.float32))).astype(jnp.bfloat16)
    return jnp.dot(readout, output_projection, preferred_element_type=jnp.float32).astype(jnp.bfloat16)

def expert_half(second_micro_input, expert_norm_gain, token_group_index, token_expert_pair, group_router_scores, expert_router_scores, expert_gate_weight, expert_up_weight, expert_down_weight):
    count = second_micro_input.shape[0]
    features = second_micro_input.astype(jnp.float32)
    centred = features - lax.optimization_barrier(jnp.mean(features, -1, keepdims=True))
    normed_input = (centred * lax.rsqrt(lax.optimization_barrier(jnp.mean(centred * centred, -1, keepdims=True)) + NORM_EPS) * expert_norm_gain).astype(jnp.bfloat16)
    group_prob = jax.nn.softmax(group_router_scores, axis=-1)
    chosen = lax.optimization_barrier(jnp.sum(jnp.where(jnp.arange(GROUPS)[None, :] == token_group_index[:, None], group_prob, 0.0), -1))
    pair_weight = jnp.stack([jax.nn.sigmoid(expert_router_scores[:, 0] - expert_router_scores[:, 1]), jax.nn.sigmoid(expert_router_scores[:, 1] - expert_router_scores[:, 0])], -1) * chosen[:, None]
    expert_id = (token_group_index[:, None] * GROUP_EXP + token_expert_pair).reshape(-1).astype(jnp.int32)
    order = jnp.argsort(expert_id, stable=True).astype(jnp.int32)
    per_expert = order.reshape(EXPERTS, -1)
    shard_width = FF // N_TP

    def one_expert(packed):
        copy_ids, gate_weight, up_weight, down_weight = packed
        rows_in = normed_input[copy_ids // 2]
        gate_terms = jnp.dot(rows_in, gate_weight, preferred_element_type=jnp.float32)
        up_terms = jnp.dot(rows_in, up_weight, preferred_element_type=jnp.float32)
        hidden = (jax.nn.silu(gate_terms) * up_terms).astype(jnp.bfloat16)
        pieces = jnp.einsum('msf,sfd->smd', hidden.reshape(-1, N_TP, shard_width).astype(jnp.float32), down_weight.reshape(N_TP, shard_width, D).astype(jnp.float32))
        rounded = lax.optimization_barrier(pieces.astype(jnp.bfloat16))
        return lax.optimization_barrier(jnp.sum(rounded.astype(jnp.float32), axis=0)).astype(jnp.bfloat16)
    outputs = lax.map(one_expert, (per_expert, expert_gate_weight, expert_up_weight, expert_down_weight))
    copies = jnp.zeros((2 * count, D), jnp.bfloat16).at[per_expert.reshape(-1)].set(outputs.reshape(-1, D))
    copies = copies.reshape(count, 2, D).astype(jnp.float32)
    return lax.optimization_barrier(jnp.sum(copies * pair_weight[:, :, None], axis=1)).astype(jnp.bfloat16)

def reference(queries, values, forget_gate_logits, output_gate_logits, forget_gate_headroom, spike_log_decay, head_norm_gain, output_projection, second_micro_input, expert_norm_gain, token_group_index, token_expert_pair, group_router_scores, expert_router_scores, expert_gate_weight, expert_up_weight, expert_down_weight):
    recurrence_output = recurrence_portion(queries, values, forget_gate_logits, output_gate_logits, forget_gate_headroom, spike_log_decay, head_norm_gain, output_projection)
    expert_tokens = expert_half(second_micro_input, expert_norm_gain, token_group_index, token_expert_pair, group_router_scores, expert_router_scores, expert_gate_weight, expert_up_weight, expert_down_weight)
    return (recurrence_output, expert_tokens)
```

```python
import functools

import jax
import jax.numpy as jnp
from jax import lax
from jax.experimental import pallas as pl
from jax.experimental.pallas import tpu as pltpu
from jax.sharding import PartitionSpec as P

HEAD_DIM = 128
GROUP_EXP = 4
BLOCK = 64
STATE_ROWS = HEAD_DIM + 16


HEAD_EPS = 1e-06
NORM_EPS = 1e-05
FULL_PRECISION = lax.Precision.HIGHEST
VMEM = pl.BlockSpec(memory_space=pltpu.VMEM)
SMEM = pl.BlockSpec(memory_space=pltpu.SMEM)
F32 = jnp.float32
BF16 = jnp.bfloat16


def nt_dot(a, b):
    return lax.dot_general(a, b, (((1,), (1,)), ((), ())), preferred_element_type=F32)


def tn_dot(a, b):
    return lax.dot_general(a, b, (((0,), (0,)), ((), ())), preferred_element_type=F32)


def scan_kernel(
    q_ref, v_ref, logit_ref, headroom_ref, spike_ref,
    local_f, local_b, reach_f, reach_b, packed_ref, state, total
):
    rows, width = q_ref.shape
    heads = width // HEAD_DIM
    blocks = rows // BLOCK
    state[...] = jnp.zeros_like(state)
    total[...] = jnp.zeros_like(total)
    row_id = lax.broadcasted_iota(jnp.int32, (BLOCK, BLOCK), 0)
    col_id = lax.broadcasted_iota(jnp.int32, (BLOCK, BLOCK), 1)
    masks = (col_id <= row_id, col_id >= row_id)

    def step(i, carry):
        for way, local, reach in ((0, local_f, reach_f), (1, local_b, reach_b)):
            block = i if way == 0 else blocks - 1 - i
            at = pl.ds(pl.multiple_of(block * BLOCK, BLOCK), BLOCK)
            queries = q_ref[at, :].astype(F32)
            lifted = queries * jax.nn.sigmoid(queries)
            inputs = v_ref[at, :]
            key = headroom_ref[way : way + 1, :] * jax.nn.sigmoid(
                -logit_ref[way, at, :].astype(F32)
            )
            decay = jnp.log1p(-key) + spike_ref[at, :]
            running = jnp.dot(
                jnp.where(masks[way], 1.0, 0.0), decay,
                precision=FULL_PRECISION, preferred_element_type=F32,
            )
            last = running[BLOCK - 1 : BLOCK] if way == 0 else running[0:1]
            middle = running[BLOCK // 2 - 1 : BLOCK // 2]
            if way == 1:
                middle = running[BLOCK // 2 : BLOCK // 2 + 1]
            query_up = (lifted * jnp.exp(running - middle)).astype(BF16)
            key_down = (key * jnp.exp(middle - running)).astype(BF16)
            key_end = (key * jnp.exp(last - running)).astype(BF16)
            query_run = (lifted * jnp.exp(running)).astype(BF16)
            sofar = total[way : way + 1, :]
            reach[at, :] = (lifted * jnp.exp(running + sofar)).astype(BF16)
            total[way : way + 1, :] = sofar + last
            shrink = jnp.exp(last)
            for head in range(heads):
                lane = slice(head * HEAD_DIM, (head + 1) * HEAD_DIM)
                scores = nt_dot(query_up[:, lane], key_down[:, lane])
                scores = jnp.where(masks[way], scores, 0.0).astype(BF16)
                held = state[way, head]
                local[at, lane] = jnp.dot(
                    scores, inputs[:, lane], preferred_element_type=F32
                ) + nt_dot(query_run[:, lane], held.astype(BF16))
                state[way, head] = shrink[:, lane] * held + tn_dot(
                    inputs[:, lane], key_end[:, lane]
                )
        return carry

    lax.fori_loop(0, blocks, step, 0)
    for way in range(2):
        for head in range(heads):
            lane = slice(head * HEAD_DIM, (head + 1) * HEAD_DIM)
            packed_ref[way, head, :HEAD_DIM, :] = state[way, head].astype(BF16)
            packed_ref[way, head, HEAD_DIM:, :] = jnp.broadcast_to(
                jnp.exp(total[way : way + 1, lane]), (STATE_ROWS - HEAD_DIM, HEAD_DIM)
            ).astype(BF16)


def readout_kernel(
    count, own_ref, local_f, local_b, reach_f, reach_b, gate_ref, gain_ref, *rest
):
    packed, out_ref, entering = rest[:count], rest[count], rest[count + 1]
    rows, width = local_f.shape
    heads = width // HEAD_DIM
    own = own_ref[0]
    for head in range(heads):
        for way in range(2):
            carried = jnp.zeros((HEAD_DIM, HEAD_DIM), F32)
            order = range(count, 0, -1) if way == 0 else range(1, count + 1)
            for away in order:
                piece = packed[away - 1][way, head].astype(F32)
                counts = away <= own if way == 0 else away > own
                joined_state = piece[HEAD_DIM : HEAD_DIM + 1] * carried + piece[:HEAD_DIM]
                carried = jnp.where(counts, joined_state, carried)
            entering[way, head] = carried.astype(BF16)
    tile = 128 if rows % 128 == 0 else BLOCK

    def step(i, carry):
        at = pl.ds(pl.multiple_of(i * tile, tile), tile)
        for head in range(heads):
            lane = slice(head * HEAD_DIM, (head + 1) * HEAD_DIM)
            joined = (
                local_f[at, lane]
                + local_b[at, lane]
                + nt_dot(reach_f[at, lane], entering[0, head])
                + nt_dot(reach_b[at, lane], entering[1, head])
            )
            normed = joined * lax.rsqrt(
                jnp.mean(joined * joined, -1, keepdims=True) + HEAD_EPS
            )
            gate = gate_ref[at, lane].astype(F32)
            out_ref[at, lane] = (
                normed * gain_ref[:, lane] * (gate * jax.nn.sigmoid(gate))
            ).astype(BF16)
        return carry

    lax.fori_loop(0, rows // tile, step, 0)


def prepare_kernel(capacity, experts, half_ref, x_ref, gain_ref, expert_ref, base_ref, *rest):
    outs, slot_ref, normed = rest[:-2], rest[-2], rest[-1]
    rows, features = x_ref.shape
    part = features // 2
    half = pl.ds(pl.multiple_of(half_ref[0] * part, part), part)
    tile = 32

    def norm_step(i, carry):
        at = pl.ds(pl.multiple_of(i * tile, tile), tile)
        x = x_ref[at, :].astype(F32)
        mean = jnp.mean(x, -1, keepdims=True)
        centred = x - mean
        scale = lax.rsqrt(jnp.mean(centred * centred, -1, keepdims=True) + NORM_EPS)
        kept = x_ref[at, half].astype(F32) - mean
        normed[at, :] = (kept * scale * gain_ref[:, half]).astype(BF16)
        return carry

    lax.fori_loop(0, rows // tile, norm_step, 0, unroll=2)
    expert_row = lax.broadcasted_iota(jnp.int32, (experts, rows), 0)
    first = expert_row == expert_ref[0:1, :]
    second = expert_row == expert_ref[1:2, :]
    named = jnp.where(first | second, 1.0, 0.0).astype(BF16)
    earlier = jnp.where(
        lax.broadcasted_iota(jnp.int32, (rows, rows), 0)
        < lax.broadcasted_iota(jnp.int32, (rows, rows), 1),
        1.0, 0.0,
    ).astype(BF16)
    rank = jnp.dot(named, earlier, preferred_element_type=F32)
    slots = []
    for k, mine in enumerate((first, second)):
        own_rank = jnp.sum(jnp.where(mine, rank, 0.0), 0, keepdims=True)
        slots.append(base_ref[k : k + 1, :] + own_rank.astype(jnp.int32))
        slot_ref[k : k + 1, :] = slots[k]
    per_device = outs[0].shape[0]
    slot_row = lax.broadcasted_iota(jnp.int32, (capacity, rows), 0)
    for away, out in enumerate(outs):
        for e in range(per_device):
            here = slot_row + (away * per_device + e) * capacity
            pick = jnp.where((here == slots[0]) | (here == slots[1]), 1.0, 0.0).astype(BF16)
            out[e] = jnp.dot(pick, normed[...], preferred_element_type=F32).astype(BF16)


def expert_kernel(count, half_ref, gate_w, up_w, down_w, *rest):
    mine, other, out_ref, x = rest[:count], rest[count : 2 * count], rest[-2], rest[-1]
    capacity, part = mine[0].shape[1:]
    own = half_ref[0]
    own_half = pl.ds(pl.multiple_of(own * part, part), part)
    other_half = pl.ds(pl.multiple_of((1 - own) * part, part), part)
    for d in range(count):
        at = slice(d * capacity, (d + 1) * capacity)
        x[at, own_half] = mine[d][0]
        x[at, other_half] = other[d][0]
    group = 2 if count % 2 == 0 else 1
    tile = group * capacity

    def step(i, carry):
        rows = x[pl.ds(pl.multiple_of(i * tile, tile), tile), :]
        gate = jnp.dot(rows, gate_w[0], preferred_element_type=F32)
        up = jnp.dot(rows, up_w[0], preferred_element_type=F32)
        hidden = (gate * jax.nn.sigmoid(gate) * up).astype(BF16)
        result = jnp.dot(hidden, down_w[0], preferred_element_type=F32).astype(BF16)
        for j in range(group):
            out_ref[i * group + j, 0] = result[j * capacity : (j + 1) * capacity]
        return carry

    lax.fori_loop(0, count // group, step, 0)


def combine_kernel(slot_ref, weight_ref, *rest):
    returned, out_ref = rest[:-1], rest[-1]
    rows = out_ref.shape[0]
    size = returned[0].shape[0]
    tile = 128 if rows % 128 == 0 else BLOCK

    def step(i, carry):
        at = pl.ds(pl.multiple_of(i * tile, tile), tile)
        column = lax.broadcasted_iota(jnp.int32, (tile, size), 1)
        sums = 0.0
        for k in range(2):
            slot = slot_ref[at, k : k + 1]
            copy = 0.0
            for d, block in enumerate(returned):
                pick = jnp.where(column + d * size == slot, 1.0, 0.0).astype(BF16)
                copy = copy + jnp.dot(pick, block[...], preferred_element_type=F32)
            sums = sums + copy * weight_ref[at, k : k + 1]
        out_ref[at, :] = sums.astype(BF16)
        return carry

    lax.fori_loop(0, rows // tile, step, 0)


def shape(dims, kind):
    return jax.ShapeDtypeStruct(dims, kind)


def cost(flops, moved):
    return pl.CostEstimate(flops=int(flops), bytes_accessed=int(moved), transcendentals=0)


def settings(mib):
    return pltpu.CompilerParams(vmem_limit_bytes=mib * 1024 * 1024)


def on_device(
    queries,
    values,
    forget_gate_logits,
    output_gate_logits,
    forget_gate_headroom,
    spike_log_decay,
    head_norm_gain,
    output_projection,
    second_micro_input,
    expert_norm_gain,
    token_group_index,
    token_expert_pair,
    group_router_scores,
    expert_router_scores,
    expert_gate_weight,
    expert_up_weight,
    expert_down_weight,
):
    rows, width = queries.shape
    heads = width // HEAD_DIM
    ep_size, tp_size = lax.axis_size("ep"), lax.axis_size("tp")
    own = lax.axis_index("ep")
    own_ref = own.astype(jnp.int32).reshape(1)
    half = (lax.axis_index("tp") % 2).astype(jnp.int32).reshape(1)

    def onward(array, away):
        return lax.ppermute(array, "ep", [(i, (i + away) % ep_size) for i in range(ep_size)])

    def swapped(array):
        return lax.ppermute(array, "tp", [(i, i ^ 1) for i in range(tp_size)])

    local_f, local_b, reach_f, reach_b, packed = pl.pallas_call(
        scan_kernel,
        out_shape=(
            shape((rows, width), F32),
            shape((rows, width), F32),
            shape((rows, width), BF16),
            shape((rows, width), BF16),
            shape((2, heads, STATE_ROWS, HEAD_DIM), BF16),
        ),
        in_specs=[VMEM] * 5,
        out_specs=[VMEM] * 5,
        scratch_shapes=[
            pltpu.VMEM((2, heads, HEAD_DIM, HEAD_DIM), F32),
            pltpu.VMEM((2, width), F32),
        ],
        compiler_params=settings(24),
        cost_estimate=cost(12e9, 8e6),
        name="scan",
    )(queries, values, forget_gate_logits, forget_gate_headroom, spike_log_decay[:, None])
    states = [onward(packed, away) for away in range(1, ep_size)]

    group_count = group_router_scores.shape[1]
    experts = group_count * GROUP_EXP
    per_device = expert_gate_weight.shape[0]
    capacity = 2 * rows // experts
    features = second_micro_input.shape[1]
    expert_id = token_group_index[None, :] * GROUP_EXP + token_expert_pair.T
    base = (
        ((expert_id // per_device - own) % ep_size) * per_device + expert_id % per_device
    ) * capacity
    inputs, _ = lax.optimization_barrier((second_micro_input, packed))
    *outgoing, slots = pl.pallas_call(
        functools.partial(prepare_kernel, capacity, experts),
        out_shape=tuple(
            [shape((per_device, capacity, features // 2), BF16)] * ep_size
            + [shape((2, rows), jnp.int32)]
        ),
        in_specs=[SMEM] + [VMEM] * 4,
        out_specs=[VMEM] * (ep_size + 1),
        scratch_shapes=[pltpu.VMEM((rows, features // 2), BF16)],
        compiler_params=settings(32),
        cost_estimate=cost(8e9, 8e6),
        name="prepare",
    )(half, inputs, expert_norm_gain[None, :], expert_id, base)
    mine = [outgoing[0]] + [onward(outgoing[d], d) for d in range(1, ep_size)]
    other = [swapped(piece) for piece in mine]

    readout = pl.pallas_call(
        functools.partial(readout_kernel, ep_size - 1),
        out_shape=shape((rows, width), BF16),
        in_specs=[SMEM] + [VMEM] * (6 + ep_size - 1),
        out_specs=VMEM,
        scratch_shapes=[pltpu.VMEM((2, heads, HEAD_DIM, HEAD_DIM), BF16)],
        compiler_params=settings(24),
        cost_estimate=cost(3e9, 4e6),
        name="readout",
    )(
        own_ref, local_f, local_b, reach_f, reach_b, output_gate_logits,
        head_norm_gain[None, :], *states
    )
    recurrence_output = jnp.dot(
        lax.all_gather(readout, "tp", axis=1, tiled=True),
        output_projection,
        preferred_element_type=F32,
    ).astype(BF16)

    group_prob = jax.nn.softmax(group_router_scores, axis=-1)
    chosen = jnp.sum(
        jnp.where(jnp.arange(group_count)[None, :] == token_group_index[:, None], group_prob, 0.0),
        -1,
    )
    pair_weight = jax.nn.sigmoid(
        expert_router_scores - jnp.flip(expert_router_scores, -1)
    ) * chosen[:, None]

    hidden_width = expert_gate_weight.shape[2]
    piece_spec = pl.BlockSpec((1, capacity, features // 2), lambda e: (e, 0, 0))
    partial_value = pl.pallas_call(
        functools.partial(expert_kernel, ep_size),
        grid=(per_device,),
        out_shape=shape((ep_size, per_device, capacity, features), BF16),
        in_specs=[
            SMEM,
            pl.BlockSpec((1, features, hidden_width), lambda e: (e, 0, 0)),
            pl.BlockSpec((1, features, hidden_width), lambda e: (e, 0, 0)),
            pl.BlockSpec((1, hidden_width, features), lambda e: (e, 0, 0)),
        ]
        + [piece_spec] * (2 * ep_size),
        out_specs=pl.BlockSpec(
            (ep_size, 1, capacity, features), lambda e: (0, e, 0, 0)
        ),
        scratch_shapes=[pltpu.VMEM((ep_size * capacity, features), BF16)],
        compiler_params=settings(50),
        cost_estimate=cost(10e9, 25e6),
        name="experts",
    )(half, expert_gate_weight, expert_up_weight, expert_down_weight, *mine, *other)
    summed = lax.psum_scatter(partial_value, "tp", scatter_dimension=3, tiled=True)
    pieces = summed.reshape(ep_size, per_device * capacity, -1)
    returned = [pieces[0]] + [onward(pieces[d], ep_size - d) for d in range(1, ep_size)]
    expert_tokens = pl.pallas_call(
        combine_kernel,
        out_shape=shape((rows, width), BF16),
        in_specs=[VMEM] * (2 + ep_size),
        out_specs=VMEM,
        compiler_params=settings(24),
        cost_estimate=cost(3e9, 3e6),
        name="combine",
    )(slots.T, pair_weight, *returned)
    return (recurrence_output, expert_tokens)


def solution(mesh):
    in_specs = (
        P("ep", "tp"),
        P("ep", "tp"),
        P(None, "ep", "tp"),
        P("ep", "tp"),
        P(None, "tp"),
        P("ep"),
        P("tp"),
        P(None, "tp"),
        P("ep", None),
        P(),
        P("ep"),
        P("ep", None),
        P("ep", None),
        P("ep", None),
        P("ep", None, "tp"),
        P("ep", None, "tp"),
        P("ep", "tp", None),
    )
    out_specs = (P("ep", "tp"), P("ep", "tp"))
    return jax.shard_map(
        on_device, mesh=mesh, in_specs=in_specs, out_specs=out_specs, check_vma=False
    )
```
